32 devices in a mesh: kv: 8 (over z, y), tp: 4 (over x, core).
Axes of the slice: x: 2, y: 2, z: 4, core: 2. Of those that a mesh axis runs over, the one named last changes fastest.
Arguments:
- tokens: bfloat16 [3072, 2048], P('kv'), may hold values from -40 to 40
- w_query: bfloat16 [2048, 2048], P(None, 'tp'), may hold values from -0.125 to 0.125
- w_key: bfloat16 [2048, 256], replicated, may hold values from -0.125 to 0.125
- w_value: bfloat16 [2048, 256], replicated, may hold values from -0.125 to 0.125
- w_out: bfloat16 [2048, 2048], P(None, 'tp'), may hold values from -0.125 to 0.125
- chosen: int32 [48, 32], P('kv'), may hold values from -1 to 46, as said below
Outputs:
- mixed: bfloat16 [3072, 2048], P('kv', 'tp')
The draws below stay inside these ranges and needn't reach their ends.
Inputs may be any that keep to these rules, and one draw needn't show every extreme that they name: `chosen`: row b lists min(b, 32) different blocks below b, block b - 1 among them when b > 0, and -1 in its other entries.
All inputs are finite; a program needn't handle non-finite values.
Results may differ from the reference program's by a relative error of at most 0.015.
The reference program's roundings to bfloat16 on the way (of `query`, `keys`, `values`, `probs`, `part` and `attention`) count: a program that leaves them out, or rounds other values in their place, can miss the bound.
Values may be sent and summed in bfloat16 or wider, within the bound.
A program may use at most 128 MiB of HBM per device.

```python
import jax
import jax.numpy as jnp
from jax import lax

D = 2048
H = 16
DH = 128
KVH = 2
BLK = 64
NSEL = 32
SEQ = 3072
NB = 48
N_TP = 4


def draw_tokens(key, part):
    base = jax.random.normal(key, (SEQ, D), jnp.float32)
    return jnp.clip(base, -40.0, 40.0).astype(jnp.bfloat16)


def draw_chosen(key, part):
    tile_tally = NB
    tile_ordinal = jnp.arange(tile_tally, dtype=jnp.int32)
    jitter_sample = jax.random.randint(key, (tile_tally, tile_tally), 0, 65536, dtype=jnp.int32)
    favoured_tiles = jax.random.randint(jax.random.fold_in(key, 7), (tile_tally,), 0, 4, dtype=jnp.int32) == 0
    merit_increment = jnp.where(favoured_tiles[None, :], 131072, 0) + jnp.where(tile_ordinal[None, :] == tile_ordinal[:, None] - 1, 262144, 0)
    preceding_tiles = tile_ordinal[None, :] < tile_ordinal[:, None]
    tile_merit = jnp.where(preceding_tiles, (jitter_sample + merit_increment) * tile_tally + tile_ordinal[None, :], -1 - tile_ordinal[None, :])
    tops, picks = lax.top_k(tile_merit, NSEL)
    return jnp.where(tops >= 0, picks, -1).astype(jnp.int32)


def level_of(own_key, shape, pieces, least, largest):
    def one(axis_at, blocks):
        draws = jax.random.uniform(jax.random.fold_in(jax.random.fold_in(own_key, 6), axis_at), (blocks,), jnp.float32, least / len(pieces), largest / len(pieces))
        return jnp.repeat(jnp.exp(draws), shape[axis_at] // blocks).reshape((-1,) + (1,) * (len(shape) - axis_at - 1))

    level = one(*pieces[0])
    for cut in pieces[1:]:
        level = level * one(*cut)
    return level


def gaussian(rng, extent, deviation, reach, pieces=(), kind=jnp.bfloat16):
    gain = level_of(rng, extent, pieces, -0.22, 0.18) if pieces else 1.0
    values = jax.random.normal(rng, extent, jnp.float32) * deviation * gain
    return jnp.minimum(jnp.maximum(values, -reach), reach).astype(kind)


def setup_inputs(seed: int = 0) -> dict:
    seeds = jax.random.split(jax.random.key(seed), 7)
    return {
        "tokens": draw_tokens(jax.random.fold_in(seeds[6], 71), 0),
        "w_query": gaussian(seeds[1], (D, H * DH), D ** -0.5, 0.125, ((1, 4),)),
        "w_key": gaussian(seeds[2], (D, KVH * DH), D ** -0.5, 0.125),
        "w_value": gaussian(seeds[3], (D, KVH * DH), D ** -0.5, 0.125),
        "w_out": gaussian(seeds[4], (H * DH, D), (H * DH) ** -0.5, 0.125, ((1, 4),)),
        "chosen": draw_chosen(jax.random.fold_in(seeds[6], 71), 0),
    }


theta_base = 10000.0


def rotate(values, positions):
    half = values.shape[-1] // 2
    inverse = theta_base ** (-jnp.arange(half, dtype=jnp.float32) / half)
    angles = positions.astype(jnp.float32)[:, None] * inverse[None, :]
    cosine = jnp.cos(angles)[:, None, :]
    sine = jnp.sin(angles)[:, None, :]
    first = values[..., :half]
    second = values[..., half:]
    return jnp.concatenate([first * cosine - second * sine, second * cosine + first * sine], axis=-1)


def reference(tokens, w_query, w_key, w_value, w_out, chosen):
    seq = tokens.shape[0]
    positions = jnp.arange(seq, dtype=jnp.int32)
    query = rotate(jnp.dot(tokens, w_query, preferred_element_type=jnp.float32).reshape(seq, H, DH), positions).astype(jnp.bfloat16)
    keys = rotate(jnp.dot(tokens, w_key, preferred_element_type=jnp.float32).reshape(seq, KVH, DH), positions).astype(jnp.bfloat16)
    values = jnp.dot(tokens, w_value, preferred_element_type=jnp.float32).astype(jnp.bfloat16).reshape(seq, KVH, DH)
    nblocks = seq // BLK
    group = H // KVH
    split = BLK // N_TP
    slots = NSEL + 1
    key_blocks = keys.reshape(nblocks, BLK, KVH, DH)
    value_blocks = values.reshape(nblocks, BLK, KVH, DH)
    query_blocks = query.reshape(nblocks, BLK, KVH, group, DH)
    lists = jnp.concatenate([chosen, jnp.arange(nblocks, dtype=jnp.int32)[:, None]], axis=1)
    scale = DH ** -0.5

    def one_block(index):
        tile_ordinal = lists[index]
        safe = jnp.maximum(tile_ordinal, 0)
        picked_keys = key_blocks[safe].astype(jnp.float32)
        picked_values = value_blocks[safe].astype(jnp.float32)
        rows = query_blocks[index].astype(jnp.float32)
        scores = jnp.einsum('qkgd,srkd->kgqsr', rows, picked_keys) * scale
        query_pos = index * BLK + jnp.arange(BLK, dtype=jnp.int32)
        key_pos = safe[:, None] * BLK + jnp.arange(BLK, dtype=jnp.int32)[None, :]
        allowed = (tile_ordinal[:, None] >= 0)[None, :, :] & (key_pos[None, :, :] <= query_pos[:, None, None])
        scores = jnp.where(allowed[None, None], scores, -jnp.inf)
        top = jnp.max(scores, axis=(3, 4), keepdims=True)
        weights = jnp.where(allowed[None, None], jnp.exp(scores - top), 0.0)
        total = jnp.sum(weights, axis=(3, 4))
        probs = lax.optimization_barrier(weights.astype(jnp.bfloat16)).astype(jnp.float32)
        probs = probs.reshape(KVH, group, BLK, slots, N_TP, split)
        grouped = picked_values.reshape(slots, N_TP, split, KVH, DH)
        parts = jnp.einsum('kgqsnr,snrkd->nqkgd', probs, grouped)
        parts = lax.optimization_barrier(parts.astype(jnp.bfloat16)).astype(jnp.float32)
        summed = jnp.sum(parts, axis=0)
        result = summed / jnp.transpose(total, (2, 0, 1))[..., None]
        return result.astype(jnp.bfloat16).reshape(BLK, H * DH)

    attention = lax.map(one_block, jnp.arange(nblocks, dtype=jnp.int32)).reshape(seq, H * DH)
    return jnp.dot(attention, w_out, preferred_element_type=jnp.float32).astype(jnp.bfloat16)
```

```python
import functools
import math

import jax
import jax.numpy as jnp
from jax import lax
from jax.experimental import pallas as pl
from jax.experimental.pallas import tpu as pltpu
from jax.sharding import PartitionSpec as P

H = 16
DH = 128
KVH = 2
BLK = 64
NSEL = 32
GROUPS = 4

theta_base = 10000.0
MESH = pl.DeviceIdType.MESH


def rotary_tables(rows, kv_index):
    half = DH // 2
    positions = kv_index * rows + jnp.arange(rows, dtype=jnp.int32)
    inverse = theta_base ** (-jnp.arange(half, dtype=jnp.float32) / half)
    angles = positions.astype(jnp.float32)[:, None] * inverse[None, :]
    cosine = jnp.cos(angles)
    sine = jnp.sin(angles)
    return jnp.concatenate([cosine, cosine], axis=1), jnp.concatenate([-sine, sine], axis=1)


def kernel(
    kv_n, tp_n,
    tokens_hbm, wq_hbm, wk_hbm, wv_hbm, wo_hbm, cos_ref, sin_ref, chosen_ref,
    out_ref,
    tokens, wq, wkv, wo, kv_all, q_all, s_ref, own_ref, vexp, att,
    in_sem, kv_send, kv_recv, att_send, att_fwd, att_recv,
):
    rows, width = tokens.shape
    own = wq.shape[1] // DH
    blocks = rows // BLK
    split = BLK // GROUPS
    out_cols = wo.shape[1]
    qrows = own * BLK
    j = lax.axis_index("kv")
    t = lax.axis_index("tp")
    core = lax.rem(t, 2)
    chip = lax.div(t, 2)
    partner = t + 1 - 2 * core
    y = lax.rem(j, 2)
    z = lax.div(j, 2)
    other = j + 1 - 2 * y
    has_next = j + 2 < kv_n
    has_prev = j >= 2
    head = lax.div(t * own, H // KVH)
    chips = tp_n // 2

    column = pl.ds(pl.multiple_of(head * DH, DH), DH)
    in_copies = [
        pltpu.make_async_copy(tokens_hbm, tokens, in_sem.at[0]),
        pltpu.make_async_copy(wk_hbm.at[:, column], wkv.at[:, pl.ds(0, DH)], in_sem.at[1]),
        pltpu.make_async_copy(wv_hbm.at[:, column], wkv.at[:, pl.ds(DH, DH)], in_sem.at[2]),
        pltpu.make_async_copy(wq_hbm, wq, in_sem.at[3]),
        pltpu.make_async_copy(wo_hbm, wo, in_sem.at[4]),
    ]
    for copy in in_copies:
        copy.start()

    barrier = pltpu.get_barrier_semaphore()

    def greet(kv_at, tp_at):
        pl.semaphore_signal(barrier, inc=1, device_id=(kv_at, tp_at), device_id_type=MESH)

    greet(other, t)
    greet(j, partner)
    for step in range(1, chips):
        greet(j, lax.rem(chip + step, chips) * 2 + core)

    @pl.when(has_next)
    def _():
        greet(j + 2, t)

    @pl.when(has_prev)
    def _():
        greet(j - 2, t)

    expected = 2 + chips - 1 + has_next.astype(jnp.int32) + has_prev.astype(jnp.int32)

    def chunk_copy(c, kind, kv_at):
        where = kv_all.at[core, pl.ds(c * blocks, blocks)]
        return pltpu.make_async_remote_copy(
            src_ref=where, dst_ref=where, send_sem=kv_send.at[kind, c], recv_sem=kv_recv.at[0, c],
            device_id=(kv_at, t), device_id_type=MESH,
        )

    def swap_copy(c):
        where = kv_all.at[core, pl.ds(c * blocks, blocks)]
        return pltpu.make_async_remote_copy(
            src_ref=where, dst_ref=where, send_sem=kv_send.at[2, c], recv_sem=kv_recv.at[1, c],
            device_id=(j, partner), device_id_type=MESH,
        )

    for copy in in_copies[:3]:
        copy.wait()
    tall = rows // 2 if blocks % 2 == 0 else rows
    tall_blocks = tall // BLK

    def project_kv(i, _):
        at = pl.multiple_of(i * tall, BLK)
        kv = jnp.dot(tokens[pl.ds(at, tall), :], wkv[...], preferred_element_type=jnp.float32)
        k = kv[:, :DH]
        k = k * cos_ref[pl.ds(at, tall), :] + pltpu.roll(k, DH // 2, 1) * sin_ref[pl.ds(at, tall), :]
        dst = pl.ds(j * blocks + i * tall_blocks, tall_blocks)
        shape = (tall_blocks, GROUPS, split, DH)
        kv_all[0, dst] = k.astype(jnp.bfloat16).reshape(shape)
        kv_all[1, dst] = kv[:, DH:].astype(jnp.bfloat16).reshape(shape)
        return 0

    lax.fori_loop(0, rows // tall, project_kv, 0)

    pl.semaphore_wait(barrier, expected)

    @pl.when(has_next)
    def _():
        chunk_copy(j, 0, j + 2).start()

    @pl.when(y == 0)
    def _():
        chunk_copy(j, 1, other).start()

    in_copies[3].wait()

    def project_q(i, _):
        at = pl.multiple_of(i * tall, BLK)
        x = tokens[pl.ds(at, tall), :]
        cosine = cos_ref[pl.ds(at, tall), :]
        sine = sin_ref[pl.ds(at, tall), :]
        for pair in range(own // 2):
            q2 = jnp.dot(x, wq[:, pair * 2 * DH:(pair + 1) * 2 * DH], preferred_element_type=jnp.float32)
            for k in range(2):
                q = q2[:, k * DH:(k + 1) * DH]
                q = (q * cosine + pltpu.roll(q, DH // 2, 1) * sine).astype(jnp.bfloat16)
                h = pair * 2 + k
                for n in range(tall_blocks):
                    q_all[i * tall_blocks + n, h * BLK:(h + 1) * BLK, :] = q[n * BLK:(n + 1) * BLK, :]
        return 0

    lax.fori_loop(0, rows // tall, project_q, 0)

    def relay_y(m):
        c = other - 2 * m
        chunk_copy(c, 1, other).wait_recv()
        swap_copy(c).start()

    @pl.when(y == 1)
    def _():
        relay_y(0)

    def relay(m, _):
        c = j - 2 * m
        chunk_copy(c, 0, other).wait_recv()

        @pl.when(has_next)
        def _():
            chunk_copy(c, 0, j + 2).start()

        chunk_copy(c, 1, other).start()
        swap_copy(c).start()
        relay_y(m)
        return 0

    lax.fori_loop(1, z + 1, relay, 0)

    def take(c, _):
        there = kv_all.at[1 - core, pl.ds(c * blocks, blocks)]
        pltpu.make_async_remote_copy(
            src_ref=there, dst_ref=there, send_sem=kv_send.at[2, c], recv_sem=kv_recv.at[1, c],
            device_id=(j, partner), device_id_type=MESH,
        ).wait_recv()
        return 0

    lax.fori_loop(0, j, take, 0)

    factor = DH ** -0.5 * math.log2(math.e)
    wide = NSEL * split

    def att_copy(source, n, sem, tp_at):
        where = att.at[source, pl.ds(pl.multiple_of(n * BLK, BLK), BLK)]
        return pltpu.make_async_remote_copy(
            src_ref=where, dst_ref=where, send_sem=sem, recv_sem=att_recv.at[source, n],
            device_id=(j, tp_at), device_id_type=MESH,
        )

    def peer(step):
        return lax.rem(chip + step, chips) * 2 + core

    def send_att(n):
        att_copy(t, n, att_send.at[0, n], partner).start()
        for step in range(1, chips):
            att_copy(t, n, att_send.at[step, n], peer(step)).start()

    def forward_att(n):
        for step in range(1, chips):
            source = peer(step)
            att_copy(source, n, att_fwd.at[step, n], partner).wait_recv()
            att_copy(source, n, att_fwd.at[step, n], partner).start()

    def attend(n, _):
        b = j * blocks + n
        valid = jnp.minimum(b, NSEL)
        index = [chosen_ref[n, s] for s in range(NSEL)]
        q = q_all[n]
        nt = (((1,), (1,)), ((), ()))
        so = lax.dot_general(q, kv_all[0, b].reshape(BLK, DH), nt, preferred_element_type=jnp.float32)
        qpos = lax.rem(lax.broadcasted_iota(jnp.int32, (qrows, BLK), 0), BLK)
        kpos = lax.broadcasted_iota(jnp.int32, (qrows, BLK), 1)
        so = jnp.where(kpos <= qpos, so, -jnp.inf)
        own_ref[...] = so
        slot = lax.div(lax.broadcasted_iota(jnp.int32, (1, wide), 1), split)
        bias = jnp.where(slot < valid, 0.0, -jnp.inf).astype(jnp.float32)
        running = None
        for g in range(GROUPS):
            k = jnp.concatenate(
                [kv_all[0, i, g] for i in index], axis=0
            )
            s = lax.dot_general(q, k, nt, preferred_element_type=jnp.float32) + bias
            s_ref[g] = s
            for piece in range(wide // DH):
                tile = s[:, piece * DH:(piece + 1) * DH]
                running = tile if running is None else jnp.maximum(running, tile)
        top = jnp.maximum(
            jnp.max(running, axis=1, keepdims=True), jnp.max(so, axis=1, keepdims=True)
        )
        po = jnp.exp2((own_ref[...] - top) * factor)
        total = jnp.sum(po, axis=1, keepdims=True)
        vo = kv_all[1, b].reshape(BLK, DH)
        for g in range(GROUPS):
            vexp[g * split:(g + 1) * split, g * DH:(g + 1) * DH] = vo[g * split:(g + 1) * split, :]
        from_own = jnp.dot(po.astype(jnp.bfloat16), vexp[...], preferred_element_type=jnp.float32)
        sums = None
        summed = None
        for g in range(GROUPS):
            v = jnp.concatenate(
                [kv_all[1, i, g] for i in index], axis=0
            )
            p = jnp.exp2((s_ref[g] - top) * factor)
            for piece in range(wide // DH):
                tile = p[:, piece * DH:(piece + 1) * DH]
                sums = tile if sums is None else sums + tile
            part = jnp.dot(p.astype(jnp.bfloat16), v, preferred_element_type=jnp.float32)
            part = (part + from_own[:, g * DH:(g + 1) * DH]).astype(jnp.bfloat16).astype(jnp.float32)
            summed = part if summed is None else summed + part
        total = total + jnp.sum(sums, axis=1, keepdims=True)
        a = (summed / total).astype(jnp.bfloat16)
        for h in range(own):
            att[t, pl.ds(pl.multiple_of(n * BLK, BLK), BLK), h * DH:(h + 1) * DH] = a[h * BLK:(h + 1) * BLK, :]
        send_att(n)

        @pl.when(n >= 1)
        def _():
            forward_att(n - 1)

        return 0

    vexp[...] = jnp.zeros_like(vexp)
    lax.fori_loop(0, blocks, attend, 0)
    forward_att(blocks - 1)

    in_copies[4].wait()

    def arrive(n, _):
        for c in range(chips):
            source = c * 2 + 1 - core
            att_copy(source, n, att_fwd.at[0, n], partner).wait_recv()
        return 0

    lax.fori_loop(0, blocks, arrive, 0)

    def project_out(i, _):
        at = pl.multiple_of(i * tall, BLK)
        step = min(out_cols, 256)
        for part in range(out_cols // step):
            acc = None
            for source in range(tp_n):
                term = jnp.dot(
                    att[source, pl.ds(at, tall), :],
                    wo[source * own * DH:(source + 1) * own * DH, part * step:(part + 1) * step],
                    preferred_element_type=jnp.float32,
                )
                acc = term if acc is None else acc + term
            out_ref[pl.ds(at, tall), part * step:(part + 1) * step] = acc.astype(jnp.bfloat16)
        return 0

    lax.fori_loop(0, rows // tall, project_out, 0)

    @pl.when(has_next)
    def _():
        chunk_copy(j, 0, j + 2).wait_send()

    @pl.when(y == 0)
    def _():
        chunk_copy(j, 1, other).wait_send()

    @pl.when(y == 1)
    def _():
        swap_copy(other).wait_send()

    def drain(m, _):
        c = j - 2 * m

        @pl.when(has_next)
        def _():
            chunk_copy(c, 0, j + 2).wait_send()

        chunk_copy(c, 1, other).wait_send()
        swap_copy(c).wait_send()
        swap_copy(other - 2 * m).wait_send()
        return 0

    lax.fori_loop(1, z + 1, drain, 0)

    def drain_att(n, _):
        att_copy(t, n, att_send.at[0, n], partner).wait_send()
        for step in range(1, chips):
            att_copy(t, n, att_send.at[step, n], peer(step)).wait_send()
            att_copy(peer(step), n, att_fwd.at[step, n], partner).wait_send()
        return 0

    lax.fori_loop(0, blocks, drain_att, 0)


def body(kv_n, tp_n, tokens, w_query, w_key, w_value, w_out, chosen):
    rows, width = tokens.shape
    own_cols = w_query.shape[1]
    own = own_cols // DH
    blocks = rows // BLK
    cosine, sine = rotary_tables(rows, lax.axis_index("kv"))
    number = (lax.axis_index("kv") * blocks + jnp.arange(blocks, dtype=jnp.int32))[:, None]
    slot = jnp.arange(NSEL, dtype=jnp.int32)[None, :]
    listed = jnp.where(number <= NSEL, slot, chosen)
    listed = jnp.where(slot < number, listed, 0)
    anywhere = pl.BlockSpec(memory_space=pl.ANY)
    vmem = pl.BlockSpec(memory_space=pltpu.VMEM)
    bf16 = jnp.bfloat16
    chips = tp_n // 2
    return pl.pallas_call(
        functools.partial(kernel, kv_n, tp_n),
        name="sparse_attention",
        out_shape=jax.ShapeDtypeStruct((rows, w_out.shape[1]), bf16),
        in_specs=[anywhere] * 5 + [vmem] * 2 + [pl.BlockSpec(memory_space=pltpu.SMEM)],
        out_specs=vmem,
        scratch_shapes=[
            pltpu.VMEM((rows, width), bf16),
            pltpu.VMEM(w_query.shape, bf16),
            pltpu.VMEM((width, 2 * DH), bf16),
            pltpu.VMEM(w_out.shape, bf16),
            pltpu.VMEM((2, kv_n * blocks, GROUPS, BLK // GROUPS, DH), bf16),
            pltpu.VMEM((blocks, own * BLK, DH), bf16),
            pltpu.VMEM((GROUPS, own * BLK, NSEL * BLK // GROUPS), jnp.float32),
            pltpu.VMEM((own * BLK, BLK), jnp.float32),
            pltpu.VMEM((BLK, GROUPS * DH), bf16),
            pltpu.VMEM((tp_n, rows, own_cols), bf16),
            pltpu.SemaphoreType.DMA((5,)),
            pltpu.SemaphoreType.DMA((3, kv_n)),
            pltpu.SemaphoreType.DMA((2, kv_n)),
            pltpu.SemaphoreType.DMA((chips, blocks)),
            pltpu.SemaphoreType.DMA((chips, blocks)),
            pltpu.SemaphoreType.DMA((tp_n, blocks)),
        ],
        compiler_params=pltpu.CompilerParams(
            collective_id=0, has_side_effects=True, vmem_limit_bytes=56 * 1024 * 1024
        ),
    )(tokens, w_query, w_key, w_value, w_out, cosine, sine, listed)


def solution(mesh):
    placed = (P("kv", None), P(None, "tp"), P(), P(), P(None, "tp"), P("kv", None))
    return jax.shard_map(
        functools.partial(body, mesh.shape["kv"], mesh.shape["tp"]),
        mesh=mesh, in_specs=placed, out_specs=P("kv", "tp"), check_vma=False,
    )
```

```python
import functools
import math

import jax
import jax.numpy as jnp
from jax import lax
from jax.experimental import pallas as pl
from jax.experimental.pallas import tpu as pltpu
from jax.sharding import PartitionSpec as P

H = 16
DH = 128
KVH = 2
BLK = 64
NSEL = 32
GROUPS = 4

theta_base = 10000.0
MESH = pl.DeviceIdType.MESH


def kernel(
    kv_n, tp_n,
    tokens_hbm, wq_hbm, wk_hbm, wv_hbm, wo_hbm, inverse_ref, chosen_ref,
    out_ref,
    tokens, wq, wkv, wo, cos_ref, sin_ref, k_all, v_all, q_all, s_ref, own_ref, top_ref, vexp, att,
    in_sem, z_send, y_send, swap_send, kv_recv, att_send, att_fwd, att_recv,
):
    rows, width = tokens.shape
    own = wq.shape[1] // DH
    blocks = rows // BLK
    half_blocks = blocks // 2
    tall = rows // 2
    split = BLK // GROUPS
    out_cols = wo.shape[1]
    qrows = own * BLK
    zn = kv_n // 2
    j = lax.axis_index("kv")
    t = lax.axis_index("tp")
    core = lax.rem(t, 2)
    chip = lax.div(t, 2)
    partner = t + 1 - 2 * core
    y = lax.rem(j, 2)
    z = lax.div(j, 2)
    other = j + 1 - 2 * y
    later = zn - 1 - z
    head = lax.div(t * own, H // KVH)
    chips = tp_n // 2

    column = pl.ds(pl.multiple_of(head * DH, DH), DH)
    first_half = pl.ds(pl.multiple_of(core * tall, BLK), tall)
    second_half = pl.ds(pl.multiple_of((1 - core) * tall, BLK), tall)
    in_copies = [
        pltpu.make_async_copy(tokens_hbm.at[first_half], tokens.at[first_half], in_sem.at[0]),
        pltpu.make_async_copy(wk_hbm.at[:, column], wkv.at[:, pl.ds(0, DH)], in_sem.at[1]),
        pltpu.make_async_copy(wv_hbm.at[:, column], wkv.at[:, pl.ds(DH, DH)], in_sem.at[2]),
        pltpu.make_async_copy(tokens_hbm.at[second_half], tokens.at[second_half], in_sem.at[3]),
        pltpu.make_async_copy(wq_hbm, wq, in_sem.at[4]),
        pltpu.make_async_copy(wo_hbm, wo, in_sem.at[5]),
    ]
    for copy in in_copies[:3]:
        copy.start()

    barrier = pltpu.get_barrier_semaphore()

    def greet(kv_at, tp_at):
        pl.semaphore_signal(barrier, inc=1, device_id=(kv_at, tp_at), device_id_type=MESH)

    greet(other, t)
    greet(j, partner)
    for step in range(1, chips):
        greet(j, lax.rem(chip + step, chips) * 2 + core)

    def greet_z(d, _):
        greet(lax.rem(z + d, zn) * 2 + y, t)
        return 0

    lax.fori_loop(1, zn, greet_z, 0)

    def part_of(kind, c, side):
        return (k_all, v_all)[kind].at[pl.ds(c * blocks + side * half_blocks, half_blocks)]

    def z_copy(kind, d):
        where = part_of(kind, j, core)
        return pltpu.make_async_remote_copy(
            src_ref=where, dst_ref=where, send_sem=z_send.at[kind, d], recv_sem=kv_recv.at[kind, 0, j],
            device_id=(j + 2 * d, t), device_id_type=MESH,
        )

    def y_copy(kind, c):
        where = part_of(kind, c, core)
        return pltpu.make_async_remote_copy(
            src_ref=where, dst_ref=where, send_sem=y_send.at[kind, c], recv_sem=kv_recv.at[kind, 0, c],
            device_id=(other, t), device_id_type=MESH,
        )

    def swap_copy(kind, c, side):
        where = part_of(kind, c, side)
        return pltpu.make_async_remote_copy(
            src_ref=where, dst_ref=where, send_sem=swap_send.at[kind, c], recv_sem=kv_recv.at[kind, 1, c],
            device_id=(j, partner), device_id_type=MESH,
        )

    lane = lax.broadcasted_iota(jnp.int32, (BLK, DH), 1)

    def tables(i, _):
        at = pl.ds(pl.multiple_of(i * BLK, BLK), BLK)
        position = (j * rows + i * BLK + lax.broadcasted_iota(jnp.int32, (BLK, DH), 0)).astype(jnp.float32)
        angle = position * inverse_ref[...]
        cos_ref[at, :] = jnp.cos(angle)
        sine = jnp.sin(angle)
        sin_ref[at, :] = jnp.where(lane < DH // 2, -sine, sine)
        return 0

    lax.fori_loop(0, blocks, tables, 0)

    def project_kv(side):
        at = pl.multiple_of(side * tall, BLK)
        kv = jnp.dot(tokens[pl.ds(at, tall), :], wkv[...], preferred_element_type=jnp.float32)
        k = kv[:, :DH]
        k = k * cos_ref[pl.ds(at, tall), :] + pltpu.roll(k, DH // 2, 1) * sin_ref[pl.ds(at, tall), :]
        dst = pl.ds(j * blocks + side * half_blocks, half_blocks)
        shape = (half_blocks, GROUPS, split, DH)
        k_all[dst] = k.astype(jnp.bfloat16).reshape(shape)
        v_all[dst] = kv[:, DH:].astype(jnp.bfloat16).reshape(shape)

    for copy in in_copies[:3]:
        copy.wait()
    for copy in in_copies[3:]:
        copy.start()
    project_kv(core)
    pl.semaphore_wait(barrier, 2 + chips - 1 + zn - 1)
    for kind in range(2):
        @pl.when(y == 0)
        def _():
            y_copy(kind, j).start()

        def send_z(i, _):
            z_copy(kind, later - i).start()
            return 0

        lax.fori_loop(0, later, send_z, 0)
    in_copies[3].wait()
    project_kv(1 - core)

    in_copies[4].wait()

    def project_q(i, _):
        at = pl.multiple_of(i * tall, BLK)
        x = tokens[pl.ds(at, tall), :]
        cosine = cos_ref[pl.ds(at, tall), :]
        sine = sin_ref[pl.ds(at, tall), :]
        for pair in range(own // 2):
            q2 = jnp.dot(x, wq[:, pair * 2 * DH:(pair + 1) * 2 * DH], preferred_element_type=jnp.float32)
            for k in range(2):
                q = q2[:, k * DH:(k + 1) * DH]
                q = (q * cosine + pltpu.roll(q, DH // 2, 1) * sine).astype(jnp.bfloat16)
                h = pair * 2 + k
                for n in range(half_blocks):
                    q_all[i * half_blocks + n, h * BLK:(h + 1) * BLK, :] = q[n * BLK:(n + 1) * BLK, :]
        return 0

    lax.fori_loop(0, 2, project_q, 0)

    def relay_y(kind, m):
        c = other - 2 * m
        y_copy(kind, c).wait_recv()
        swap_copy(kind, c, core).start()

    def relay_first(kind):
        @pl.when(y == 1)
        def _():
            relay_y(kind, 0)

    def relay(kind, m):
        c = j - 2 * m
        y_copy(kind, c).wait_recv()
        y_copy(kind, c).start()
        swap_copy(kind, c, core).start()

        @pl.when(m >= 2)
        def _():
            relay_y(kind, m - 1)

        @pl.when(m == z)
        def _():
            relay_y(kind, m)

    def relay_keys(m, _):
        relay(0, m)
        return 0

    def take(kind):
        def one(c, _):
            swap_copy(kind, c, 1 - core).wait_recv()
            return 0

        lax.fori_loop(0, j, one, 0)

    relay_first(0)
    lax.fori_loop(1, z + 1, relay_keys, 0)
    take(0)

    factor = DH ** -0.5 * math.log2(math.e)
    wide = NSEL * split

    def att_copy(source, n, sem, tp_at):
        where = att.at[source, pl.ds(pl.multiple_of(n * BLK, BLK), BLK)]
        return pltpu.make_async_remote_copy(
            src_ref=where, dst_ref=where, send_sem=sem, recv_sem=att_recv.at[source, n],
            device_id=(j, tp_at), device_id_type=MESH,
        )

    def peer(step):
        return lax.rem(chip + step, chips) * 2 + core

    def send_att(n):
        for step in range(1, chips):
            att_copy(t, n, att_send.at[step, n], peer(step)).start()
        att_copy(t, n, att_send.at[0, n], partner).start()

    def forward_att(n):
        for step in range(1, chips):
            source = peer(step)
            att_copy(source, n, att_fwd.at[step, n], partner).wait_recv()
            att_copy(source, n, att_fwd.at[step, n], partner).start()

    def block_index(n):
        b = j * blocks + n
        many = (b > NSEL).astype(jnp.int32)
        last = jnp.maximum(b - 1, 0)
        return [many * chosen_ref[n, s] + (1 - many) * jnp.minimum(s, last) for s in range(NSEL)]

    def score(n):
        b = j * blocks + n
        index = block_index(n)
        q = q_all[n]
        nt = (((1,), (1,)), ((), ()))
        so = lax.dot_general(q, k_all[b].reshape(BLK, DH), nt, preferred_element_type=jnp.float32)
        qpos = lax.rem(lax.broadcasted_iota(jnp.int32, (qrows, BLK), 0), BLK)
        kpos = lax.broadcasted_iota(jnp.int32, (qrows, BLK), 1)
        so = jnp.where(kpos <= qpos, so, -jnp.inf)
        own_ref[n] = so
        slot = lax.div(lax.broadcasted_iota(jnp.int32, (1, wide), 1), split)
        bias = jnp.where(slot < b, 0.0, -jnp.inf).astype(jnp.float32)
        running = None
        for g in range(GROUPS):
            k = jnp.concatenate([k_all[i, g] for i in index], axis=0)
            s = lax.dot_general(q, k, nt, preferred_element_type=jnp.float32) + bias
            s_ref[n, g] = s
            for piece in range(wide // DH):
                tile = s[:, piece * DH:(piece + 1) * DH]
                running = tile if running is None else jnp.maximum(running, tile)
        top = jnp.maximum(
            jnp.max(running, axis=1, keepdims=True), jnp.max(so, axis=1, keepdims=True)
        )
        top_ref[n] = jnp.broadcast_to(top, (qrows, DH))

    def attend(n):
        b = j * blocks + n
        index = block_index(n)
        top = top_ref[n][:, :1]
        po = jnp.exp2((own_ref[n] - top) * factor)
        total = jnp.sum(po, axis=1, keepdims=True)
        vo = v_all[b].reshape(BLK, DH)
        for g in range(GROUPS):
            vexp[g * split:(g + 1) * split, g * DH:(g + 1) * DH] = vo[g * split:(g + 1) * split, :]
        from_own = jnp.dot(po.astype(jnp.bfloat16), vexp[...], preferred_element_type=jnp.float32)
        sums = None
        summed = None
        for g in range(GROUPS):
            v = jnp.concatenate([v_all[i, g] for i in index], axis=0)
            p = jnp.exp2((s_ref[n, g] - top) * factor)
            for piece in range(wide // DH):
                tile = p[:, piece * DH:(piece + 1) * DH]
                sums = tile if sums is None else sums + tile
            part = jnp.dot(p.astype(jnp.bfloat16), v, preferred_element_type=jnp.float32)
            part = (part + from_own[:, g * DH:(g + 1) * DH]).astype(jnp.bfloat16).astype(jnp.float32)
            summed = part if summed is None else summed + part
        total = total + jnp.sum(sums, axis=1, keepdims=True)
        a = (summed / total).astype(jnp.bfloat16)
        for h in range(own):
            att[t, pl.ds(pl.multiple_of(n * BLK, BLK), BLK), h * DH:(h + 1) * DH] = a[h * BLK:(h + 1) * BLK, :]
        send_att(n)

        @pl.when(n >= 1)
        def _():
            forward_att(n - 1)

    ahead = half_blocks
    per = -(-(zn - 1) // ahead)

    def lead(n, _):
        score(n)

        @pl.when(n == 0)
        def _():
            relay_first(1)

        for k in range(per):
            m = n * per + k + 1

            @pl.when(m <= z)
            def _():
                relay(1, m)

        return 0

    def follow(n, _):
        attend(n)
        score(n + ahead)
        return 0

    def finish(n, _):
        attend(n)
        return 0

    vexp[...] = jnp.zeros_like(vexp)
    lax.fori_loop(0, ahead, lead, 0)
    take(1)
    lax.fori_loop(0, blocks - ahead, follow, 0)
    lax.fori_loop(blocks - ahead, blocks, finish, 0)
    forward_att(blocks - 1)

    in_copies[5].wait()

    def arrive(n, _):
        for c in range(chips):
            source = c * 2 + 1 - core
            att_copy(source, n, att_fwd.at[0, n], partner).wait_recv()
        return 0

    lax.fori_loop(0, blocks, arrive, 0)

    def project_out(i, _):
        at = pl.multiple_of(i * tall, BLK)
        step = min(out_cols, 256)
        for part in range(out_cols // step):
            acc = None
            for source in range(tp_n):
                term = jnp.dot(
                    att[source, pl.ds(at, tall), :],
                    wo[source * own * DH:(source + 1) * own * DH, part * step:(part + 1) * step],
                    preferred_element_type=jnp.float32,
                )
                acc = term if acc is None else acc + term
            out_ref[pl.ds(at, tall), part * step:(part + 1) * step] = acc.astype(jnp.bfloat16)
        return 0

    lax.fori_loop(0, rows // tall, project_out, 0)

    for kind in range(2):
        @pl.when(y == 0)
        def _():
            y_copy(kind, j).wait_send()

        def drain_z(i, _):
            z_copy(kind, i + 1).wait_send()
            return 0

        def drain_y(m, _):
            y_copy(kind, j - 2 * m).wait_send()
            return 0

        def drain_swap(c, _):
            swap_copy(kind, c, core).wait_send()
            return 0

        lax.fori_loop(0, later, drain_z, 0)
        lax.fori_loop(1, z + 1, drain_y, 0)
        lax.fori_loop(0, j, drain_swap, 0)

    def drain_att(n, _):
        att_copy(t, n, att_send.at[0, n], partner).wait_send()
        for step in range(1, chips):
            att_copy(t, n, att_send.at[step, n], peer(step)).wait_send()
            att_copy(peer(step), n, att_fwd.at[step, n], partner).wait_send()
        return 0

    lax.fori_loop(0, blocks, drain_att, 0)


def body(kv_n, tp_n, tokens, w_query, w_key, w_value, w_out, chosen):
    rows, width = tokens.shape
    own_cols = w_query.shape[1]
    own = own_cols // DH
    blocks = rows // BLK
    half = DH // 2
    inverse = theta_base ** (-jnp.arange(half, dtype=jnp.float32) / half)
    inverse = jnp.concatenate([inverse, inverse])[None, :]
    anywhere = pl.BlockSpec(memory_space=pl.ANY)
    vmem = pl.BlockSpec(memory_space=pltpu.VMEM)
    bf16 = jnp.bfloat16
    chips = tp_n // 2
    return pl.pallas_call(
        functools.partial(kernel, kv_n, tp_n),
        name="sparse_attention",
        out_shape=jax.ShapeDtypeStruct((rows, w_out.shape[1]), bf16),
        in_specs=[anywhere] * 5 + [vmem] + [pl.BlockSpec(memory_space=pltpu.SMEM)],
        out_specs=vmem,
        scratch_shapes=[
            pltpu.VMEM((rows, width), bf16),
            pltpu.VMEM(w_query.shape, bf16),
            pltpu.VMEM((width, 2 * DH), bf16),
            pltpu.VMEM(w_out.shape, bf16),
            pltpu.VMEM((rows, DH), jnp.float32),
            pltpu.VMEM((rows, DH), jnp.float32),
            pltpu.VMEM((kv_n * blocks, GROUPS, BLK // GROUPS, DH), bf16),
            pltpu.VMEM((kv_n * blocks, GROUPS, BLK // GROUPS, DH), bf16),
            pltpu.VMEM((blocks, own * BLK, DH), bf16),
            pltpu.VMEM((blocks, GROUPS, own * BLK, NSEL * BLK // GROUPS), jnp.float32),
            pltpu.VMEM((blocks, own * BLK, BLK), jnp.float32),
            pltpu.VMEM((blocks, own * BLK, DH), jnp.float32),
            pltpu.VMEM((BLK, GROUPS * DH), bf16),
            pltpu.VMEM((tp_n, rows, own_cols), bf16),
            pltpu.SemaphoreType.DMA((6,)),
            pltpu.SemaphoreType.DMA((2, kv_n // 2)),
            pltpu.SemaphoreType.DMA((2, kv_n)),
            pltpu.SemaphoreType.DMA((2, kv_n)),
            pltpu.SemaphoreType.DMA((2, 2, kv_n)),
            pltpu.SemaphoreType.DMA((chips, blocks)),
            pltpu.SemaphoreType.DMA((chips, blocks)),
            pltpu.SemaphoreType.DMA((tp_n, blocks)),
        ],
        compiler_params=pltpu.CompilerParams(
            collective_id=0, has_side_effects=True, vmem_limit_bytes=56 * 1024 * 1024
        ),
    )(tokens, w_query, w_key, w_value, w_out, inverse, chosen)


def solution(mesh):
    placed = (P("kv", None), P(None, "tp"), P(), P(), P(None, "tp"), P("kv", None))
    return jax.shard_map(
        functools.partial(body, mesh.shape["kv"], mesh.shape["tp"]),
        mesh=mesh, in_specs=placed, out_specs=P("kv", "tp"), check_vma=False,
    )
```
